32 devices in a mesh: kv: 8 (over z, x), tp: 4 (over y, core).
Axes of the slice: x: 2, y: 2, z: 4, core: 2. Of those that a mesh axis runs over, the one named last changes fastest.
Arguments:
- hidden_in: bfloat16 [16, 4096], P(None, ('kv', 'tp')), may hold values from -5 to 5
- pre_gain: float32 [4096], P('kv'), may hold values from 0.1 to 1.9
- w_query: bfloat16 [4096, 3072], P('kv', 'tp'), may hold values from -0.09375 to 0.09375
- w_key: bfloat16 [4096, 1024], P('kv', 'tp'), may hold values from -0.09375 to 0.09375
- w_value: bfloat16 [4096, 1024], P('kv', 'tp'), may hold values from -0.09375 to 0.09375
- w_forget: bfloat16 [4096, 16], P('kv'), may hold values from -0.09375 to 0.09375
- forget_bias: float32 [16], P('tp'), may hold values from -2 to 1.5
- key_cache: bfloat16 [16, 8192, 1024], P(None, 'kv', 'tp'), may hold values from -1300 to 1300
- value_cache: bfloat16 [16, 8192, 1024], P(None, 'kv', 'tp'), may hold values from -6 to 6
- decay_to_end: float32 [16, 16, 8192], P(None, 'tp', 'kv'), may hold values from -8194 to 0, as said below
- w_output: bfloat16 [3072, 4096], P('tp', 'kv'), may hold values from -0.109375 to 0.109375
- mid_gain: float32 [4096], P('kv'), may hold values from 0.1 to 1.9
- w_gate: bfloat16 [4096, 11264], P('kv', 'tp'), may hold values from -0.09375 to 0.09375
- w_up: bfloat16 [4096, 11264], P('kv', 'tp'), may hold values from -0.09375 to 0.09375
- w_down: bfloat16 [11264, 4096], P('tp', 'kv'), may hold values from -0.0546875 to 0.0546875
Outputs:
- updated: float32 [16, 4096], P(None, ('kv', 'tp'))
The draws below stay inside these ranges and needn't reach their ends.
Inputs may be any that keep to these rules, and one draw needn't show every extreme that they name: `decay_to_end`: never falls toward later positions and is 0 at the last cached position.
All inputs are finite; a program needn't handle non-finite values.
Results may differ from the reference program's by a relative error of at most 0.028.
Values may be sent and summed in bfloat16 or wider, within the bound.
A program may use at most 128 MiB of HBM per device.

```python
import jax
import jax.numpy as jnp
from jax import lax

D = 4096
QH = 48
KEY_VALUE_HEADS = 16
HD = 64
FF = 11264
BATCH_SEQUENCES = 16
POS_DEV = 1024
CACHE_LENGTH = 8192
N_KV = 8
N_TP = 4


def draw_hidden_in(key, part):
    key_base, key_rough = jax.random.split(key, 2)
    column = jnp.arange(D).astype(jnp.float32)
    span = D // N_KV
    rise = column / D + column % span / span
    rough = jnp.exp(jax.random.uniform(key_rough, (D,), minval=-0.7, maxval=0.7))
    scale = jnp.exp(jnp.log(3.0) * rise) * rough
    base = jnp.clip(jax.random.normal(key_base, (BATCH_SEQUENCES, D)), -5.0, 5.0)
    return (0.05 * base * scale[None, :]).astype(jnp.bfloat16)


def draw_key_cache(key, part):
    key_base = jax.random.fold_in(key, 0)
    result = jnp.clip(jax.random.normal(key_base, (BATCH_SEQUENCES, CACHE_LENGTH, KEY_VALUE_HEADS, HD)), -6.0, 6.0)
    return result.reshape(BATCH_SEQUENCES, CACHE_LENGTH, KEY_VALUE_HEADS * HD).astype(jnp.bfloat16)


def draw_decay_to_end(key, part):
    key_entries = jax.random.split(key, 7)
    slow_share = 0.5
    sluggish_flag = jax.random.uniform(key_entries[0], (KEY_VALUE_HEADS,)) < slow_share
    total = jnp.exp(jax.random.uniform(key_entries[1], (KEY_VALUE_HEADS,), minval=jnp.log(0.2), maxval=jnp.log(0.8)))
    fast_len = jnp.exp(jax.random.uniform(key_entries[2], (KEY_VALUE_HEADS,), minval=jnp.log(30.0), maxval=jnp.log(100.0)))
    mean_rate = jnp.where(sluggish_flag, total / CACHE_LENGTH, 1.0 / fast_len)
    shard_factor = jnp.exp(jax.random.uniform(key_entries[3], (BATCH_SEQUENCES, KEY_VALUE_HEADS, N_KV), minval=-0.7, maxval=0.7))
    block_of = jnp.arange(CACHE_LENGTH) // POS_DEV
    shard_pos = jnp.take(shard_factor, block_of, axis=2)
    rough = jnp.exp(jax.random.uniform(key_entries[4], (BATCH_SEQUENCES, KEY_VALUE_HEADS, CACHE_LENGTH), minval=jnp.log(0.3), maxval=jnp.log(3.0)))
    decode_steps = -mean_rate[None, :, None] * shard_pos * rough
    spike_offset = jax.random.randint(key_entries[5], (BATCH_SEQUENCES, KEY_VALUE_HEADS, 2), 0, CACHE_LENGTH)
    spike_length = jnp.log(jax.random.uniform(key_entries[6], (BATCH_SEQUENCES, KEY_VALUE_HEADS, 2), minval=0.55, maxval=0.8))
    decode_position = jnp.arange(CACHE_LENGTH)
    spike_count = jnp.where(decode_position[None, None, :] == spike_offset[:, :, 0:1], spike_length[:, :, 0:1], 0.0)
    spike_count = spike_count + jnp.where(decode_position[None, None, :] == spike_offset[:, :, 1:2], spike_length[:, :, 1:2], 0.0)
    decode_steps = decode_steps + jnp.where(sluggish_flag[None, :, None], spike_count, 0.0)
    later = jnp.cumsum(decode_steps[:, :, ::-1], axis=2)[:, :, ::-1] - decode_steps
    return later.astype(jnp.float32)


def steps_of(own_key, dims, shards, low, top_value):
    gain, own = 1.0, jax.random.fold_in(own_key, 6)
    for position, blocks in shards:
        heights = jnp.exp(jax.random.uniform(jax.random.fold_in(own, position), (blocks,), jnp.float32, low / len(shards), top_value / len(shards)))
        gain = gain * jnp.repeat(heights, dims[position] // blocks).reshape([-1 if axis == position else 1 for axis in range(len(dims))])
    return gain


def centred(key, dims, width, reach, cuts=(), kind=jnp.bfloat16):
    values = jax.random.normal(key, dims, jnp.float32) * width
    if len(cuts) > 0:
        values = steps_of(key, dims, cuts, -0.22, 0.18) * values
    return jnp.clip(values, min=-reach, max=reach).astype(kind)


def setup_inputs(seed: int = 0) -> dict:
    key_of = jax.random.split(jax.random.key(seed), 16)
    hidden_in = draw_hidden_in(jax.random.fold_in(key_of[15], 71), 0)
    pre_gain = jnp.clip(1.0 + 0.18 * jax.random.normal(key_of[1], (D,), jnp.float32), 0.1, 1.9)
    w_query = centred(key_of[2], (D, QH * HD), D ** -0.5, 0.09375, ((0, 8), (1, 4)))
    w_key = centred(key_of[3], (D, KEY_VALUE_HEADS * HD), D ** -0.5, 0.09375, ((0, 8), (1, 4)))
    w_value = centred(key_of[4], (D, KEY_VALUE_HEADS * HD), D ** -0.5, 0.09375, ((0, 8), (1, 4)))
    w_forget = centred(key_of[5], (D, KEY_VALUE_HEADS), D ** -0.5, 0.09375, ((0, 8),))
    forget_bias = jnp.clip(-2.0 + 3.5 * jax.random.uniform(key_of[6], (KEY_VALUE_HEADS,), jnp.float32) ** steps_of(key_of[6], (KEY_VALUE_HEADS,), ((0, 4),), -0.2, 0.2), -2.0, 1.5)
    key_cache = draw_key_cache(jax.random.fold_in(key_of[15], 71), 0)
    value_cache = centred(key_of[8], (BATCH_SEQUENCES, CACHE_LENGTH, KEY_VALUE_HEADS * HD), 1.0, 6.0, ((1, 8), (2, 4)))
    decay_to_end = draw_decay_to_end(jax.random.fold_in(key_of[15], 71), 0)
    w_output = centred(key_of[10], (QH * HD, D), (QH * HD) ** -0.5, 0.109375, ((0, 4), (1, 8)))
    mid_gain = jnp.clip(1.0 + 0.18 * jax.random.normal(key_of[11], (D,), jnp.float32), 0.1, 1.9)
    w_gate = centred(key_of[12], (D, FF), D ** -0.5, 0.09375, ((0, 8), (1, 4)))
    w_up = centred(key_of[13], (D, FF), D ** -0.5, 0.09375, ((0, 8), (1, 4)))
    w_down = centred(key_of[14], (FF, D), FF ** -0.5, 0.0546875, ((0, 4), (1, 8)))
    return {"hidden_in": hidden_in, "pre_gain": pre_gain, "w_query": w_query, "w_key": w_key, "w_value": w_value, "w_forget": w_forget, "forget_bias": forget_bias, "key_cache": key_cache, "value_cache": value_cache, "decay_to_end": decay_to_end, "w_output": w_output, "mid_gain": mid_gain, "w_gate": w_gate, "w_up": w_up, "w_down": w_down}


norm_eps = 1e-06

def grouped_sum(left, weight):
    groups = N_TP
    left_three = left.reshape(left.shape[0], groups, -1).astype(jnp.float32)
    weight_three = weight.reshape(groups, -1, weight.shape[1]).astype(jnp.float32)
    partial_terms = jnp.einsum('btk,tkd->btd', left_three, weight_three)
    rounded = lax.optimization_barrier(partial_terms.astype(jnp.bfloat16))
    return lax.optimization_barrier(jnp.sum(rounded.astype(jnp.float32), axis=1))

def attend_one(operands):
    query_b, keys_b, values_b, decay_b, key_own, value_own, log_b = operands
    score_scale = HD ** (-0.5)
    key_rows = keys_b.reshape(CACHE_LENGTH, KEY_VALUE_HEADS, HD).astype(jnp.float32)
    value_rows = values_b.reshape(CACHE_LENGTH, KEY_VALUE_HEADS, HD).astype(jnp.float32)
    query_f = query_b.astype(jnp.float32)
    scores = jnp.einsum('gqd,lgd->gql', query_f, key_rows) * score_scale
    scores = scores + log_b[:, None, None] + decay_b[:, None, :]
    own_score = jnp.einsum('gqd,gd->gq', query_f, key_own.astype(jnp.float32)) * score_scale
    largest = jnp.maximum(lax.optimization_barrier(jnp.max(scores, axis=2)), own_score)
    weights = jnp.exp(scores - largest[:, :, None])
    own_weight = jnp.exp(own_score - largest)
    total = lax.optimization_barrier(jnp.sum(weights, axis=2)) + own_weight
    rounded = lax.optimization_barrier(weights.astype(jnp.bfloat16))
    mixed = jnp.einsum('gql,lgd->gqd', rounded.astype(jnp.float32), value_rows)
    mixed = mixed + own_weight[:, :, None] * value_own.astype(jnp.float32)[:, None, :]
    return mixed / total[:, :, None]

def reference(hidden_in, pre_gain, w_query, w_key, w_value, w_forget, forget_bias, key_cache, value_cache, decay_to_end, w_output, mid_gain, w_gate, w_up, w_down):
    group_size = QH // KEY_VALUE_HEADS
    x_float = hidden_in.astype(jnp.float32)
    inv_rms = lax.rsqrt(lax.optimization_barrier(jnp.mean(x_float * x_float, axis=1, keepdims=True)) + norm_eps)
    scaled = (x_float * pre_gain).astype(jnp.bfloat16)
    query = (jnp.dot(scaled, w_query, preferred_element_type=jnp.float32) * inv_rms).astype(jnp.bfloat16)
    key_new = (jnp.dot(scaled, w_key, preferred_element_type=jnp.float32) * inv_rms).astype(jnp.bfloat16)
    value_new = (jnp.dot(scaled, w_value, preferred_element_type=jnp.float32) * inv_rms).astype(jnp.bfloat16)
    log_new = jax.nn.log_sigmoid(jnp.dot(scaled, w_forget, preferred_element_type=jnp.float32) * inv_rms + forget_bias)
    attended = lax.map(attend_one, (query.reshape(BATCH_SEQUENCES, KEY_VALUE_HEADS, group_size, HD), key_cache, value_cache, decay_to_end, key_new.reshape(BATCH_SEQUENCES, KEY_VALUE_HEADS, HD), value_new.reshape(BATCH_SEQUENCES, KEY_VALUE_HEADS, HD), log_new))
    attended = attended.reshape(BATCH_SEQUENCES, QH * HD).astype(jnp.bfloat16)
    projected = grouped_sum(attended, w_output)
    mid_float = x_float + projected
    mid_inv = lax.rsqrt(lax.optimization_barrier(jnp.mean(mid_float * mid_float, axis=1, keepdims=True)) + norm_eps)
    mid_scaled = (mid_float * mid_gain).astype(jnp.bfloat16)
    gate = jnp.dot(mid_scaled, w_gate, preferred_element_type=jnp.float32) * mid_inv
    upward = jnp.dot(mid_scaled, w_up, preferred_element_type=jnp.float32) * mid_inv
    hidden_units = (jax.nn.silu(gate) * upward).astype(jnp.bfloat16)
    lowered = grouped_sum(hidden_units, w_down)
    return mid_float + lowered
```

```python
import functools

import jax
import jax.numpy as jnp
from jax import lax
from jax.experimental import pallas as pl
from jax.experimental.pallas import tpu as pltpu
from jax.sharding import PartitionSpec as P

HD = 64
norm_eps = 1e-06
F32 = jnp.float32
BF16 = jnp.bfloat16
MESH = pl.DeviceIdType.MESH


def exchange(axis, n, me, send_sem, recv_sem, source_of, target_of):
    copies = []
    for k in range(1, n):
        peer = lax.rem(me + k, n)
        copy = pltpu.make_async_remote_copy(
            src_ref=source_of(peer),
            dst_ref=target_of(k),
            send_sem=send_sem.at[k],
            recv_sem=recv_sem.at[k],
            device_id={axis: peer},
            device_id_type=MESH,
        )
        copy.start()
        copies.append(copy)
    return copies


def layer_kernel(
    n_kv, n_tp, group, d_model,
    hid_ref, pg_ref, wf_ref, mg_ref, bias_ref,
    wq_hbm, wk_hbm, wv_hbm, kc_hbm, vc_hbm, dec_hbm, wo_hbm, wg_hbm, wu_hbm, wd_hbm,
    out_ref,
    wq, wk, wv, kc, vc, dec, wo, wg, wu, wd,
    hbuf, pbuf, prec, qbuf, qm, qbd, fold, cbuf, crec, abuf, orec, gbuf, grec, ubuf, dbuf, drec, mine,
    load_sem, wo_sem, kv_send, kv_recv, tp_send, tp_recv,
):
    mk = lax.axis_index("kv")
    mt = lax.axis_index("tp")
    batch = hid_ref.shape[0]
    lanes = hid_ref.shape[1]
    nb = batch // n_kv
    nq, nk, ff = wq.shape[1], wk.shape[1], wg.shape[1]
    kvh = nk // HD
    span = group + 1
    rows = qbd.shape[1]
    positions = kc.shape[1]

    pairs = ((wq_hbm, wq), (wk_hbm, wk), (wv_hbm, wv), (kc_hbm, kc), (dec_hbm, dec), (vc_hbm, vc),
             (wg_hbm, wg), (wu_hbm, wu), (wd_hbm, wd))
    loads = [pltpu.make_async_copy(a, b, load_sem.at[i]) for i, (a, b) in enumerate(pairs)]
    ld_q, ld_k, ld_v, ld_kc, ld_dec, ld_vc, ld_g, ld_u, ld_d = loads
    wo_loads = []
    for g in range(kvh):
        for j in range(group):
            wo_loads.append(pltpu.make_async_copy(
                wo_hbm.at[pl.ds((g * group + j) * HD, HD)],
                wo.at[pl.ds(j * nk + g * HD, HD)],
                wo_sem.at[g * group + j]))
    for c in (ld_q, ld_k, ld_v, ld_kc, ld_dec, ld_vc):
        c.start()
    for c in wo_loads:
        c.start()
    for c in (ld_g, ld_u, ld_d):
        c.start()

    barrier = pltpu.get_barrier_semaphore()
    for k in range(1, n_tp):
        pl.semaphore_signal(barrier, inc=1, device_id={"tp": lax.rem(mt + k, n_tp)}, device_id_type=MESH)
    for k in range(1, n_kv):
        pl.semaphore_signal(barrier, inc=1, device_id={"kv": lax.rem(mk + k, n_kv)}, device_id_type=MESH)
    pl.semaphore_wait(barrier, n_tp + n_kv - 2)

    pending = []
    c_h = exchange("tp", n_tp, mt, tp_send.at[0], tp_recv.at[0], lambda peer: hid_ref, lambda k: hbuf.at[mt])
    pending += c_h
    hbuf[mt] = hid_ref[...]

    col = lax.broadcasted_iota(jnp.int32, (nq, nk), 0)
    col2 = lax.broadcasted_iota(jnp.int32, (nq, nk), 1)
    head_col = sum(((col >= t * group * HD).astype(jnp.int32) for t in range(1, kvh)), jnp.zeros_like(col))
    same = ((col & (HD - 1)) == (col2 & (HD - 1))) & (head_col == lax.shift_right_logical(col2, 6))
    fold[...] = jnp.where(same, HD ** (-0.5), 0.0).astype(BF16)
    mcol = lax.broadcasted_iota(jnp.int32, (rows, nq), 1)
    mrow = lax.broadcasted_iota(jnp.int32, (rows, nq), 0)
    mhead = sum(((mcol >= t * group * HD).astype(jnp.int32) for t in range(1, kvh)), jnp.zeros_like(mcol))
    mask = (mhead * span + lax.shift_right_logical(mcol, 6) - mhead * group) == mrow
    group_of_col = lax.shift_right_logical(lax.broadcasted_iota(jnp.int32, (span, nk), 1), 6)
    span_row = lax.broadcasted_iota(jnp.int32, (span, nk), 0)
    lane_i = lax.broadcasted_iota(jnp.int32, (rows, nk), 1)
    row_i = lax.broadcasted_iota(jnp.int32, (rows, nk), 0)
    eye_max = lane_i == row_i
    eye_sum = lane_i == row_i + rows
    row_one = lax.broadcasted_iota(jnp.int32, (rows, 1), 0)
    row_group = sum(((row_one >= t * span).astype(jnp.int32) for t in range(1, kvh)), jnp.zeros_like(row_one))
    frow = lax.broadcasted_iota(jnp.int32, (rows, 128), 0)
    fgroup = sum(((frow >= t * span).astype(jnp.int32) for t in range(1, kvh)), jnp.zeros_like(frow))
    pick_forget = lax.broadcasted_iota(jnp.int32, (rows, 128), 1) == fgroup + mt * kvh
    bias = jnp.zeros((rows, 1), F32)
    for g in range(kvh):
        bias = jnp.where(row_group == g, bias_ref[g], bias)

    def collapse(x):
        total = jnp.zeros((span, nk), F32)
        for g in range(kvh):
            total = jnp.where(group_of_col == g, x[g * span:(g + 1) * span], total)
        return total

    for c in c_h:
        c.wait_recv()
    block = jnp.concatenate([hbuf[t] for t in range(n_tp)], axis=1).astype(F32)
    scaled = (block * pg_ref[...]).astype(BF16)
    square = jnp.sum(block * block, axis=1, keepdims=True)
    f_part = jnp.dot(scaled, wf_ref[...], preferred_element_type=F32)
    nf = f_part.shape[1]
    base = nq + 2 * nk
    pbuf[:, :, base:base + nf] = f_part.reshape(batch, 1, nf)
    pbuf[:, :, base + nf:] = jnp.broadcast_to(square, (batch, 128 - nf)).reshape(batch, 1, 128 - nf)
    ld_q.wait()
    pbuf[:, :, 0:nq] = jnp.dot(scaled, wq[...], preferred_element_type=F32).reshape(batch, 1, nq)
    ld_k.wait()
    pbuf[:, :, nq:nq + nk] = jnp.dot(scaled, wk[...], preferred_element_type=F32).reshape(batch, 1, nk)
    ld_v.wait()
    pbuf[:, :, nq + nk:base] = jnp.dot(scaled, wv[...], preferred_element_type=F32).reshape(batch, 1, nk)
    c_p = exchange("kv", n_kv, mk, kv_send.at[0], kv_recv.at[0],
                   lambda peer: pbuf.at[pl.ds(peer * nb, nb)], lambda k: prec.at[k])
    pending += c_p
    for c in c_p:
        c.wait_recv()
    keys_own, values_own, logs_own = [], [], []
    for i in range(nb):
        total = pbuf[mk * nb + i]
        for k in range(1, n_kv):
            total = total + prec[k, i]
        inv = lax.rsqrt(total[:, base + 127:base + 128] / d_model + norm_eps)
        qbuf[mk * nb + i] = (total[:, 0:nq] * inv).astype(BF16).astype(F32)
        keys_own.append((total[:, nq:nq + nk] * inv).astype(BF16).astype(F32))
        values_own.append((total[:, nq + nk:base] * inv).astype(BF16).astype(F32))
        forget = jnp.broadcast_to(total[:, base:base + 128] * inv, (rows, 128))
        forget = jnp.sum(jnp.where(pick_forget, forget, 0.0), axis=1, keepdims=True) + bias
        logs_own.append(jnp.minimum(forget, 0.0) - jnp.log(1.0 + jnp.exp(-jnp.abs(forget))))
    own_rows = pl.ds(mk * nb, nb)
    c_q = exchange("kv", n_kv, mk, kv_send.at[1], kv_recv.at[1],
                   lambda peer: qbuf.at[own_rows], lambda k: qbuf.at[own_rows])
    pending += c_q
    for c in c_q:
        c.wait_recv()
    for b in range(batch):
        qm[b * rows:(b + 1) * rows, :] = jnp.where(mask, jnp.broadcast_to(qbuf[b], (rows, nq)), 0.0).astype(BF16)
    qbd[...] = jnp.dot(qm[...], fold[...], preferred_element_type=F32).astype(BF16).reshape(batch, rows, nk)

    ld_kc.wait()
    ld_dec.wait()
    ld_vc.wait()

    def attend(b, carry):
        scores = lax.dot_general(qbd[b], kc[b], (((1,), (1,)), ((), ())), preferred_element_type=F32)
        decay = dec[b]
        parts = [jnp.broadcast_to(decay[g:g + 1], (span, positions)) for g in range(kvh)]
        if rows > kvh * span:
            parts.append(jnp.broadcast_to(decay[0:1], (rows - kvh * span, positions)))
        scores = scores + jnp.concatenate(parts, axis=0)
        top = jnp.max(scores, axis=1, keepdims=True)
        weights = jnp.exp(scores - top)
        total = jnp.sum(weights, axis=1, keepdims=True)
        acc = jnp.dot(weights.astype(BF16), vc[b], preferred_element_type=F32)
        stat = jnp.sum(jnp.where(eye_max, top, jnp.where(eye_sum, total, 0.0)), axis=0, keepdims=True)
        cbuf[b] = jnp.where(span_row == group, jnp.broadcast_to(stat, (span, nk)), collapse(acc))
        return carry

    lax.fori_loop(0, batch, attend, 0, unroll=4)

    c_c = exchange("kv", n_kv, mk, kv_send.at[2], kv_recv.at[2],
                   lambda peer: cbuf.at[pl.ds(peer * nb, nb)], lambda k: crec.at[k])
    pending += c_c
    for c in c_c:
        c.wait_recv()
    for i in range(nb):
        messages = [cbuf[mk * nb + i]] + [crec[k, i] for k in range(1, n_kv)]
        tops, totals = [], []
        for message in messages:
            stat = jnp.broadcast_to(message[group:group + 1], (rows, nk))
            tops.append(jnp.sum(jnp.where(eye_max, stat, 0.0), axis=1, keepdims=True) + logs_own[i])
            totals.append(jnp.sum(jnp.where(eye_sum, stat, 0.0), axis=1, keepdims=True))
        own = jnp.sum(qbd[mk * nb + i].astype(F32) * keys_own[i], axis=1, keepdims=True)
        top = functools.reduce(jnp.maximum, tops, own)
        own_weight = jnp.exp(own - top)
        factors = [jnp.exp(t - top) for t in tops]
        norm = own_weight
        for factor, total in zip(factors, totals):
            norm = norm + factor * total
        attended = collapse(jnp.broadcast_to(own_weight / norm, (rows, nk))) * values_own[i]
        for factor, message in zip(factors, messages):
            attended = attended + message * collapse(jnp.broadcast_to(factor / norm, (rows, nk)))
        attended = jnp.where(span_row == group, 0.0, attended)
        abuf[mk * nb + i] = attended.astype(BF16).astype(F32)
    c_a = exchange("kv", n_kv, mk, kv_send.at[3], kv_recv.at[3],
                   lambda peer: abuf.at[own_rows], lambda k: abuf.at[own_rows])
    pending += c_a
    for c in wo_loads:
        c.wait()
    for c in c_a:
        c.wait_recv()
    out_part = jnp.zeros((batch, wo.shape[1]), F32)
    for j in range(group):
        out_part = out_part + jnp.dot(
            abuf[:, j, :].astype(BF16), wo[j * nk:(j + 1) * nk, :], preferred_element_type=F32)
    orec[mt] = out_part.astype(BF16)
    c_o = exchange("tp", n_tp, mt, tp_send.at[1], tp_recv.at[1], lambda peer: orec.at[mt], lambda k: orec.at[mt])
    pending += c_o
    for c in c_o:
        c.wait_recv()
    projected = orec[0].astype(F32)
    for t in range(1, n_tp):
        projected = projected + orec[t].astype(F32)
    after = block + projected
    for t in range(n_tp):
        mine[t] = after[:, t * lanes:(t + 1) * lanes]
    mid = (after * mg_ref[...]).astype(BF16)
    mid_square = jnp.sum(after * after, axis=1, keepdims=True)
    ld_g.wait()
    gbuf[:, :, 0:ff] = jnp.dot(mid, wg[...], preferred_element_type=F32).reshape(batch, 1, ff)
    ld_u.wait()
    gbuf[:, :, ff:2 * ff] = jnp.dot(mid, wu[...], preferred_element_type=F32).reshape(batch, 1, ff)
    gbuf[:, :, 2 * ff:] = jnp.broadcast_to(mid_square, (batch, 128)).reshape(batch, 1, 128)
    c_g = exchange("kv", n_kv, mk, kv_send.at[4], kv_recv.at[4],
                   lambda peer: gbuf.at[pl.ds(peer * nb, nb)], lambda k: grec.at[k])
    pending += c_g
    for c in c_g:
        c.wait_recv()
    for i in range(nb):
        total = gbuf[mk * nb + i]
        for k in range(1, n_kv):
            total = total + grec[k, i]
        inv = lax.rsqrt(total[:, 2 * ff:2 * ff + 1] / d_model + norm_eps)
        gate = total[:, 0:ff] * inv
        up = total[:, ff:2 * ff] * inv
        ubuf[mk * nb + i] = gate / (1.0 + jnp.exp(-gate)) * up
    c_u = exchange("kv", n_kv, mk, kv_send.at[5], kv_recv.at[5],
                   lambda peer: ubuf.at[own_rows], lambda k: ubuf.at[own_rows])
    pending += c_u
    ld_d.wait()
    for c in c_u:
        c.wait_recv()
    units = ubuf[:, 0, :].astype(BF16)
    down = jnp.dot(units, wd[...], preferred_element_type=F32).astype(BF16)
    for t in range(n_tp):
        dbuf[t] = down[:, t * lanes:(t + 1) * lanes]
    c_d = exchange("tp", n_tp, mt, tp_send.at[2], tp_recv.at[2], lambda peer: dbuf.at[peer], lambda k: drec.at[k])
    pending += c_d
    for c in c_d:
        c.wait_recv()
    lowered = dbuf[mt].astype(F32)
    for k in range(1, n_tp):
        lowered = lowered + drec[k].astype(F32)
    out_ref[...] = mine[mt] + lowered
    for c in pending:
        c.wait_send()


def on_device(
    n_kv, n_tp,
    hidden_in, pre_gain, w_query, w_key, w_value, w_forget, forget_bias, key_cache, value_cache,
    decay_to_end, w_output, mid_gain, w_gate, w_up, w_down,
):
    batch, lanes = hidden_in.shape
    depth, nq = w_query.shape
    nk = w_key.shape[1]
    ff = w_gate.shape[1]
    kvh = decay_to_end.shape[1]
    group = nq // nk
    d_model = lanes * n_kv * n_tp
    span = group + 1
    rows = max(16, -(-kvh * span // 16) * 16)
    nb = batch // n_kv
    width = nq + 2 * nk + 128
    wide = 2 * ff + 128
    vmem = pl.BlockSpec(memory_space=pltpu.VMEM)
    anywhere = pl.BlockSpec(memory_space=pl.ANY)
    big = (w_query, w_key, w_value, key_cache, value_cache, decay_to_end, w_output, w_gate, w_up, w_down)
    scratch = [pltpu.VMEM(a.shape, a.dtype) for a in big] + [
        pltpu.VMEM((n_tp, batch, lanes), BF16),
        pltpu.VMEM((batch, 1, width), F32),
        pltpu.VMEM((n_kv, nb, 1, width), F32),
        pltpu.VMEM((batch, 1, nq), F32),
        pltpu.VMEM((batch * rows, nq), BF16),
        pltpu.VMEM((batch, rows, nk), BF16),
        pltpu.VMEM((nq, nk), BF16),
        pltpu.VMEM((batch, span, nk), F32),
        pltpu.VMEM((n_kv, nb, span, nk), F32),
        pltpu.VMEM((batch, span, nk), F32),
        pltpu.VMEM((n_tp, batch, w_output.shape[1]), BF16),
        pltpu.VMEM((batch, 1, wide), F32),
        pltpu.VMEM((n_kv, nb, 1, wide), F32),
        pltpu.VMEM((batch, 1, ff), F32),
        pltpu.VMEM((n_tp, batch, lanes), BF16),
        pltpu.VMEM((n_tp, batch, lanes), BF16),
        pltpu.VMEM((n_tp, batch, lanes), F32),
        pltpu.SemaphoreType.DMA((9,)),
        pltpu.SemaphoreType.DMA((kvh * group,)),
        pltpu.SemaphoreType.DMA((6, n_kv)),
        pltpu.SemaphoreType.DMA((6, n_kv)),
        pltpu.SemaphoreType.DMA((3, n_tp)),
        pltpu.SemaphoreType.DMA((3, n_tp)),
    ]
    return pl.pallas_call(
        functools.partial(layer_kernel, n_kv, n_tp, group, d_model),
        out_shape=jax.ShapeDtypeStruct((batch, lanes), F32),
        in_specs=[vmem] * 4 + [pl.BlockSpec(memory_space=pltpu.SMEM)] + [anywhere] * 10,
        out_specs=vmem,
        scratch_shapes=scratch,
        compiler_params=pltpu.CompilerParams(
            collective_id=0, has_side_effects=True, vmem_limit_bytes=60 * 1024 * 1024
        ),
        name="decode_layer",
    )(hidden_in, pre_gain.reshape(1, -1), w_forget, mid_gain.reshape(1, -1), forget_bias, *big)


def solution(mesh):
    in_specs = (
        P(None, ("kv", "tp")),
        P("kv"),
        P("kv", "tp"),
        P("kv", "tp"),
        P("kv", "tp"),
        P("kv", None),
        P("tp"),
        P(None, "kv", "tp"),
        P(None, "kv", "tp"),
        P(None, "tp", "kv"),
        P("tp", "kv"),
        P("kv"),
        P("kv", "tp"),
        P("kv", "tp"),
        P("tp", "kv"),
    )
    return jax.shard_map(
        functools.partial(on_device, mesh.shape["kv"], mesh.shape["tp"]),
        mesh=mesh,
        in_specs=in_specs,
        out_specs=P(None, ("kv", "tp")),
        check_vma=False,
    )
```

```python
import functools

import jax
import jax.numpy as jnp
from jax import lax
from jax.experimental import pallas as pl
from jax.experimental.pallas import tpu as pltpu
from jax.sharding import PartitionSpec as P

HD = 64
norm_eps = 1e-06
F32 = jnp.float32
BF16 = jnp.bfloat16
MESH = pl.DeviceIdType.MESH


def exchange(axis, n, me, send_sem, recv_sem, source_of, target_of, start=True):
    copies = []
    for k in range(1, n):
        peer = lax.rem(me + k, n)
        copy = pltpu.make_async_remote_copy(
            src_ref=source_of(peer),
            dst_ref=target_of(k),
            send_sem=send_sem.at[k],
            recv_sem=recv_sem.at[k],
            device_id={axis: peer},
            device_id_type=MESH,
        )
        if start:
            copy.start()
        copies.append(copy)
    return copies


def layer_kernel(
    n_kv, n_tp, group, d_model,
    hid_ref, pg_ref, wf_ref, mg_ref, bias_ref,
    wq_hbm, wk_hbm, wv_hbm, kc_hbm, vc_hbm, dec_hbm, wo_hbm, wg_hbm, wu_hbm, wd_hbm,
    out_ref,
    wq, wk, wv, kc, vc, dec, wo, wg, wu, wd,
    hbuf, pbuf, prec, qbuf, qm, qbd, fold, cbuf, crec, abuf, orec, gbuf, grec, ubuf, sq_own, srec, dbuf, drec, mine,
    load_sem, wo_sem, kv_send, kv_recv, tp_send, tp_recv,
):
    mk = lax.axis_index("kv")
    mt = lax.axis_index("tp")
    batch = hid_ref.shape[0]
    lanes = hid_ref.shape[1]
    nb = batch // n_kv
    nq, nk, ff = wq.shape[1], wk.shape[1], wg.shape[1]
    kvh = nk // HD
    span = group + 1
    rows = qbd.shape[1]
    positions = kc.shape[1]

    pairs = ((wq_hbm, wq), (wk_hbm, wk), (wv_hbm, wv), (kc_hbm, kc), (dec_hbm, dec), (vc_hbm, vc),
             (wg_hbm, wg), (wu_hbm, wu), (wd_hbm, wd))
    loads = [pltpu.make_async_copy(a, b, load_sem.at[i]) for i, (a, b) in enumerate(pairs)]
    ld_q, ld_k, ld_v, ld_kc, ld_dec, ld_vc, ld_g, ld_u, ld_d = loads
    wo_loads = []
    for g in range(kvh):
        for j in range(group):
            wo_loads.append(pltpu.make_async_copy(
                wo_hbm.at[pl.ds((g * group + j) * HD, HD)],
                wo.at[pl.ds(j * nk + g * HD, HD)],
                wo_sem.at[g * group + j]))
    for c in (ld_q, ld_k, ld_v, ld_kc, ld_dec, ld_vc):
        c.start()
    for c in wo_loads:
        c.start()
    for c in (ld_g, ld_u, ld_d):
        c.start()

    barrier = pltpu.get_barrier_semaphore()
    for k in range(1, n_tp):
        pl.semaphore_signal(barrier, inc=1, device_id={"tp": lax.rem(mt + k, n_tp)}, device_id_type=MESH)
    for k in range(1, n_kv):
        pl.semaphore_signal(barrier, inc=1, device_id={"kv": lax.rem(mk + k, n_kv)}, device_id_type=MESH)
    pl.semaphore_wait(barrier, n_tp + n_kv - 2)

    pending = []
    c_h = exchange("tp", n_tp, mt, tp_send.at[0], tp_recv.at[0], lambda peer: hid_ref, lambda k: hbuf.at[mt])
    pending += c_h
    hbuf[mt] = hid_ref[...]

    col = lax.broadcasted_iota(jnp.int32, (nq, nk), 0)
    col2 = lax.broadcasted_iota(jnp.int32, (nq, nk), 1)
    head_col = sum(((col >= t * group * HD).astype(jnp.int32) for t in range(1, kvh)), jnp.zeros_like(col))
    same = ((col & (HD - 1)) == (col2 & (HD - 1))) & (head_col == lax.shift_right_logical(col2, 6))
    fold[...] = jnp.where(same, HD ** (-0.5), 0.0).astype(BF16)
    mcol = lax.broadcasted_iota(jnp.int32, (rows, nq), 1)
    mrow = lax.broadcasted_iota(jnp.int32, (rows, nq), 0)
    mhead = sum(((mcol >= t * group * HD).astype(jnp.int32) for t in range(1, kvh)), jnp.zeros_like(mcol))
    mask = (mhead * span + lax.shift_right_logical(mcol, 6) - mhead * group) == mrow
    group_of_col = lax.shift_right_logical(lax.broadcasted_iota(jnp.int32, (span, nk), 1), 6)
    span_row = lax.broadcasted_iota(jnp.int32, (span, nk), 0)
    lane_i = lax.broadcasted_iota(jnp.int32, (rows, nk), 1)
    row_i = lax.broadcasted_iota(jnp.int32, (rows, nk), 0)
    eye_max = lane_i == row_i
    eye_sum = lane_i == row_i + rows
    row_one = lax.broadcasted_iota(jnp.int32, (rows, 1), 0)
    row_group = sum(((row_one >= t * span).astype(jnp.int32) for t in range(1, kvh)), jnp.zeros_like(row_one))
    frow = lax.broadcasted_iota(jnp.int32, (rows, 128), 0)
    fgroup = sum(((frow >= t * span).astype(jnp.int32) for t in range(1, kvh)), jnp.zeros_like(frow))
    pick_forget = lax.broadcasted_iota(jnp.int32, (rows, 128), 1) == fgroup + mt * kvh
    bias = jnp.zeros((rows, 1), F32)
    for g in range(kvh):
        bias = jnp.where(row_group == g, bias_ref[g], bias)

    def collapse(x):
        total = jnp.zeros((span, nk), F32)
        for g in range(kvh):
            total = jnp.where(group_of_col == g, x[g * span:(g + 1) * span], total)
        return total

    for c in c_h:
        c.wait_recv()
    block = jnp.concatenate([hbuf[t] for t in range(n_tp)], axis=1).astype(F32)
    scaled = (block * pg_ref[...]).astype(BF16)
    square = jnp.sum(block * block, axis=1, keepdims=True)
    f_part = lax.dot_general(scaled, wf_ref[...], (((1,), (1,)), ((), ())), preferred_element_type=F32)
    nf = f_part.shape[1]
    base = nq + 2 * nk
    pbuf[:, :, base:base + nf] = f_part.reshape(batch, 1, nf)
    pbuf[:, :, base + nf:] = jnp.broadcast_to(square, (batch, 128 - nf)).reshape(batch, 1, 128 - nf)
    ld_q.wait()
    pbuf[:, :, 0:nq] = jnp.dot(scaled, wq[...], preferred_element_type=F32).reshape(batch, 1, nq)
    ld_k.wait()
    pbuf[:, :, nq:nq + nk] = jnp.dot(scaled, wk[...], preferred_element_type=F32).reshape(batch, 1, nk)
    ld_v.wait()
    pbuf[:, :, nq + nk:base] = jnp.dot(scaled, wv[...], preferred_element_type=F32).reshape(batch, 1, nk)
    c_p = exchange("kv", n_kv, mk, kv_send.at[0], kv_recv.at[0],
                   lambda peer: pbuf.at[pl.ds(peer * nb, nb)], lambda k: prec.at[k])
    pending += c_p
    for c in c_p:
        c.wait_recv()
    keys_own, values_own, logs_own = [], [], []
    for i in range(nb):
        total = pbuf[mk * nb + i]
        for k in range(1, n_kv):
            total = total + prec[k, i]
        inv = lax.rsqrt(total[:, base + 127:base + 128] / d_model + norm_eps)
        qbuf[mk * nb + i] = (total[:, 0:nq] * inv).astype(BF16).astype(F32)
        keys_own.append((total[:, nq:nq + nk] * inv).astype(BF16).astype(F32))
        values_own.append((total[:, nq + nk:base] * inv).astype(BF16).astype(F32))
        forget = jnp.broadcast_to(total[:, base:base + 128] * inv, (rows, 128))
        forget = jnp.sum(jnp.where(pick_forget, forget, 0.0), axis=1, keepdims=True) + bias
        logs_own.append(jnp.minimum(forget, 0.0) - jnp.log(1.0 + jnp.exp(-jnp.abs(forget))))
    own_rows = pl.ds(mk * nb, nb)
    c_q = exchange("kv", n_kv, mk, kv_send.at[1], kv_recv.at[1],
                   lambda peer: qbuf.at[own_rows], lambda k: qbuf.at[own_rows])
    pending += c_q
    for c in c_q:
        c.wait_recv()
    for b in range(batch):
        qm[b * rows:(b + 1) * rows, :] = jnp.where(mask, jnp.broadcast_to(qbuf[b], (rows, nq)), 0.0).astype(BF16)
    qbd[...] = jnp.dot(qm[...], fold[...], preferred_element_type=F32).astype(BF16).reshape(batch, rows, nk)

    ld_kc.wait()
    ld_dec.wait()
    ld_vc.wait()

    def attend(b):
        scores = lax.dot_general(qbd[b], kc[b], (((1,), (1,)), ((), ())), preferred_element_type=F32)
        decay = dec[b]
        parts = [jnp.broadcast_to(decay[g:g + 1], (span, positions)) for g in range(kvh)]
        if rows > kvh * span:
            parts.append(jnp.broadcast_to(decay[0:1], (rows - kvh * span, positions)))
        scores = scores + jnp.concatenate(parts, axis=0)
        top = jnp.max(scores, axis=1, keepdims=True)
        weights = jnp.exp(scores - top)
        total = jnp.sum(weights, axis=1, keepdims=True)
        acc = jnp.dot(weights.astype(BF16), vc[b], preferred_element_type=F32)
        stat = jnp.sum(jnp.where(eye_max, top, jnp.where(eye_sum, total, 0.0)), axis=0, keepdims=True)
        cbuf[b] = jnp.where(span_row == group, jnp.broadcast_to(stat, (span, nk)), collapse(acc))

    c_c = exchange("kv", n_kv, mk, kv_send.at[2], kv_recv.at[2],
                   lambda peer: cbuf.at[pl.ds(peer * nb, nb)], lambda k: crec.at[k], start=False)
    for k in list(range(1, n_kv)) + [0]:
        for i in range(nb):
            attend(lax.rem(mk + k, n_kv) * nb + i)
        if k > 0:
            c_c[k - 1].start()
    pending += c_c
    for c in c_c:
        c.wait_recv()
    for i in range(nb):
        messages = [cbuf[mk * nb + i]] + [crec[k, i] for k in range(1, n_kv)]
        tops, totals = [], []
        for message in messages:
            stat = jnp.broadcast_to(message[group:group + 1], (rows, nk))
            tops.append(jnp.sum(jnp.where(eye_max, stat, 0.0), axis=1, keepdims=True) + logs_own[i])
            totals.append(jnp.sum(jnp.where(eye_sum, stat, 0.0), axis=1, keepdims=True))
        own = jnp.sum(qbd[mk * nb + i].astype(F32) * keys_own[i], axis=1, keepdims=True)
        top = functools.reduce(jnp.maximum, tops, own)
        own_weight = jnp.exp(own - top)
        factors = [jnp.exp(t - top) for t in tops]
        norm = own_weight
        for factor, total in zip(factors, totals):
            norm = norm + factor * total
        attended = collapse(jnp.broadcast_to(own_weight / norm, (rows, nk))) * values_own[i]
        for factor, message in zip(factors, messages):
            attended = attended + message * collapse(jnp.broadcast_to(factor / norm, (rows, nk)))
        attended = jnp.where(span_row == group, 0.0, attended)
        abuf[mk * nb + i] = attended.astype(BF16).astype(F32)
    c_a = exchange("kv", n_kv, mk, kv_send.at[3], kv_recv.at[3],
                   lambda peer: abuf.at[own_rows], lambda k: abuf.at[own_rows])
    pending += c_a
    for c in wo_loads:
        c.wait()
    for c in c_a:
        c.wait_recv()
    out_part = jnp.zeros((batch, wo.shape[1]), F32)
    for j in range(group):
        out_part = out_part + jnp.dot(
            abuf[:, j, :].astype(BF16), wo[j * nk:(j + 1) * nk, :], preferred_element_type=F32)
    orec[mt] = out_part.astype(BF16)
    c_o = exchange("tp", n_tp, mt, tp_send.at[1], tp_recv.at[1], lambda peer: orec.at[mt], lambda k: orec.at[mt])
    pending += c_o
    for c in c_o:
        c.wait_recv()
    projected = orec[0].astype(F32)
    for t in range(1, n_tp):
        projected = projected + orec[t].astype(F32)
    after = block + projected
    for t in range(n_tp):
        mine[t] = after[:, t * lanes:(t + 1) * lanes]
    mid = (after * mg_ref[...]).astype(BF16)
    mid_square = jnp.sum(after * after, axis=1, keepdims=True)
    eye = lax.broadcasted_iota(jnp.int32, (batch, 128), 0) == lax.broadcasted_iota(jnp.int32, (batch, 128), 1)
    sq_own[...] = jnp.sum(jnp.where(eye, mid_square, 0.0), axis=0, keepdims=True)
    c_s = exchange("kv", n_kv, mk, kv_send.at[6], kv_recv.at[6], lambda peer: sq_own, lambda k: srec.at[k])
    pending += c_s
    ld_g.wait()
    ld_u.wait()
    chunk = ubuf.shape[2]
    c_g = exchange("kv", n_kv, mk, kv_send.at[4], kv_recv.at[4],
                   lambda peer: gbuf.at[peer], lambda k: grec.at[k], start=False)
    pending += c_g
    for s in range(n_kv):
        low = s * chunk
        size = max(0, min(ff - low, chunk))
        for at, weight in ((0, wg), (chunk, wu)):
            if size > 0:
                gbuf[s, :, at:at + size] = jnp.dot(
                    mid, weight[:, low:low + size], preferred_element_type=F32).astype(BF16)
            if size < chunk:
                gbuf[s, :, at + size:at + chunk] = jnp.zeros((batch, chunk - size), BF16)

        @pl.when(mk != s)
        def _():
            k = lax.rem(s - mk + n_kv, n_kv)
            pltpu.make_async_remote_copy(
                src_ref=gbuf.at[s],
                dst_ref=grec.at[k],
                send_sem=kv_send.at[4, k],
                recv_sem=kv_recv.at[4, k],
                device_id={"kv": jnp.int32(s)},
                device_id_type=MESH,
            ).start()

    squares = sq_own[...]
    for k in range(1, n_kv):
        c_s[k - 1].wait_recv()
        squares = squares + srec[k]
    squares = jnp.sum(jnp.where(eye, jnp.broadcast_to(squares, eye.shape), 0.0), axis=1, keepdims=True)
    mid_inv = lax.rsqrt(squares / d_model + norm_eps)
    total = gbuf[mk].astype(F32)
    for k in range(1, n_kv):
        c_g[k - 1].wait_recv()
        total = total + grec[k].astype(F32)
    gate = total[:, 0:chunk] * mid_inv
    up = total[:, chunk:] * mid_inv
    ubuf[mk] = (gate / (1.0 + jnp.exp(-gate)) * up).astype(BF16)
    c_u = exchange("kv", n_kv, mk, kv_send.at[5], kv_recv.at[5],
                   lambda peer: ubuf.at[mk], lambda k: ubuf.at[mk])
    pending += c_u
    ld_d.wait()
    for c in c_u:
        c.wait_recv()
    down = jnp.zeros((batch, wd.shape[1]), F32)
    for s in range(n_kv):
        low = s * chunk
        size = max(0, min(ff - low, chunk))
        if size > 0:
            down = down + jnp.dot(ubuf[s][:, 0:size], wd[low:low + size, :], preferred_element_type=F32)
    down = down.astype(BF16)
    for t in range(n_tp):
        dbuf[t] = down[:, t * lanes:(t + 1) * lanes]
    c_d = exchange("tp", n_tp, mt, tp_send.at[2], tp_recv.at[2], lambda peer: dbuf.at[peer], lambda k: drec.at[k])
    pending += c_d
    for c in c_d:
        c.wait_recv()
    lowered = dbuf[mt].astype(F32)
    for k in range(1, n_tp):
        lowered = lowered + drec[k].astype(F32)
    out_ref[...] = mine[mt] + lowered
    for c in pending:
        c.wait_send()


def on_device(
    n_kv, n_tp,
    hidden_in, pre_gain, w_query, w_key, w_value, w_forget, forget_bias, key_cache, value_cache,
    decay_to_end, w_output, mid_gain, w_gate, w_up, w_down,
):
    batch, lanes = hidden_in.shape
    depth, nq = w_query.shape
    nk = w_key.shape[1]
    ff = w_gate.shape[1]
    kvh = decay_to_end.shape[1]
    group = nq // nk
    d_model = lanes * n_kv * n_tp
    span = group + 1
    rows = max(16, -(-kvh * span // 16) * 16)
    nb = batch // n_kv
    width = nq + 2 * nk + 128
    chunk = -(-ff // (128 * n_kv)) * 128
    vmem = pl.BlockSpec(memory_space=pltpu.VMEM)
    anywhere = pl.BlockSpec(memory_space=pl.ANY)
    big = (w_query, w_key, w_value, key_cache, value_cache, decay_to_end, w_output, w_gate, w_up, w_down)
    scratch = [pltpu.VMEM(a.shape, a.dtype) for a in big] + [
        pltpu.VMEM((n_tp, batch, lanes), BF16),
        pltpu.VMEM((batch, 1, width), F32),
        pltpu.VMEM((n_kv, nb, 1, width), F32),
        pltpu.VMEM((batch, 1, nq), F32),
        pltpu.VMEM((batch * rows, nq), BF16),
        pltpu.VMEM((batch, rows, nk), BF16),
        pltpu.VMEM((nq, nk), BF16),
        pltpu.VMEM((batch, span, nk), F32),
        pltpu.VMEM((n_kv, nb, span, nk), F32),
        pltpu.VMEM((batch, span, nk), F32),
        pltpu.VMEM((n_tp, batch, w_output.shape[1]), BF16),
        pltpu.VMEM((n_kv, batch, 2 * chunk), BF16),
        pltpu.VMEM((n_kv, batch, 2 * chunk), BF16),
        pltpu.VMEM((n_kv, batch, chunk), BF16),
        pltpu.VMEM((1, 128), F32),
        pltpu.VMEM((n_kv, 1, 128), F32),
        pltpu.VMEM((n_tp, batch, lanes), BF16),
        pltpu.VMEM((n_tp, batch, lanes), BF16),
        pltpu.VMEM((n_tp, batch, lanes), F32),
        pltpu.SemaphoreType.DMA((9,)),
        pltpu.SemaphoreType.DMA((kvh * group,)),
        pltpu.SemaphoreType.DMA((7, n_kv)),
        pltpu.SemaphoreType.DMA((7, n_kv)),
        pltpu.SemaphoreType.DMA((3, n_tp)),
        pltpu.SemaphoreType.DMA((3, n_tp)),
    ]
    return pl.pallas_call(
        functools.partial(layer_kernel, n_kv, n_tp, group, d_model),
        out_shape=jax.ShapeDtypeStruct((batch, lanes), F32),
        in_specs=[vmem] * 4 + [pl.BlockSpec(memory_space=pltpu.SMEM)] + [anywhere] * 10,
        out_specs=vmem,
        scratch_shapes=scratch,
        compiler_params=pltpu.CompilerParams(
            collective_id=0, has_side_effects=True, vmem_limit_bytes=60 * 1024 * 1024
        ),
        name="decode_layer",
    )(hidden_in, pre_gain.reshape(1, -1), w_forget.T, mid_gain.reshape(1, -1), forget_bias, *big)


def solution(mesh):
    in_specs = (
        P(None, ("kv", "tp")),
        P("kv"),
        P("kv", "tp"),
        P("kv", "tp"),
        P("kv", "tp"),
        P("kv", None),
        P("tp"),
        P(None, "kv", "tp"),
        P(None, "kv", "tp"),
        P(None, "tp", "kv"),
        P("tp", "kv"),
        P("kv"),
        P("kv", "tp"),
        P("kv", "tp"),
        P("tp", "kv"),
    )
    return jax.shard_map(
        functools.partial(on_device, mesh.shape["kv"], mesh.shape["tp"]),
        mesh=mesh,
        in_specs=in_specs,
        out_specs=P(None, ("kv", "tp")),
        check_vma=False,
    )
```
